32 devices in a mesh: grp: 2 (over x), kv: 4 (over y, core), tp: 4 (over z).
Axes of the slice: x: 2, y: 2, z: 4, core: 2. Of those that a mesh axis runs over, the one named last changes fastest.
Arguments:
- tokens: bfloat16 [128, 4096], P('grp', ('kv', 'tp')), parts along dimension 0, may hold values from -20 to 20, as said below
- norm_gain: bfloat16 [4096], P('kv'), may hold values from 0.099609375 to 1.8984375
- w_query: bfloat16 [4096, 2048], P('kv', 'tp'), may hold values from -0.09375 to 0.09375
- w_key: bfloat16 [4096, 2048], P('kv', 'tp'), may hold values from -0.09375 to 0.09375
- w_value: bfloat16 [4096, 4096], P('kv', 'tp'), may hold values from -0.09375 to 0.09375
- w_outgate: bfloat16 [4096, 4096], P('kv', 'tp'), may hold values from -0.09375 to 0.09375
- w_input_gate: bfloat16 [4096, 32], P('kv'), may hold values from -0.09375 to 0.09375
- w_forget_gate: bfloat16 [4096, 32], P('kv'), may hold values from -0.09375 to 0.09375
- memory: float32 [128, 32, 64, 128], P(('grp', 'kv'), 'tp'), parts along dimension 0, may hold values from -4 to 4
- normalizer: float32 [128, 32, 64], P(('grp', 'kv'), 'tp'), parts along dimension 0, may hold values from -4 to 4
- stabilizer: float32 [128, 32], P(('grp', 'kv'), 'tp'), parts along dimension 0, may hold values from -4 to 4
- w_mix_out: bfloat16 [4096, 4096], P('tp', 'kv'), may hold values from -0.09375 to 0.09375
- ffn_gain: bfloat16 [4096], P('kv'), may hold values from 0.099609375 to 1.8984375
- w_gate: bfloat16 [4096, 11264], P('kv', 'tp'), may hold values from -0.09375 to 0.09375
- w_up: bfloat16 [4096, 11264], P('kv', 'tp'), may hold values from -0.09375 to 0.09375
- w_down: bfloat16 [11264, 4096], P('tp', 'kv'), may hold values from -0.3125 to 0.3125
Outputs:
- layer_out: bfloat16 [128, 4096], P('grp', ('kv', 'tp')), parts along dimension 0
- new_memory: float32 [128, 32, 64, 128], P(('grp', 'kv'), 'tp'), parts along dimension 0
- new_normalizer: float32 [128, 32, 64], P(('grp', 'kv'), 'tp'), parts along dimension 0
- new_stabilizer: float32 [128, 32], P(('grp', 'kv'), 'tp'), parts along dimension 0
The draws below stay inside these ranges and needn't reach their ends.
There are 2 independent parts, one for each index of `grp`. The reference program is written for one: setup_inputs(seed, part) draws one part's arguments, and reference() takes and returns one part's arrays. A program takes and returns all parts, laid end to end along the dimension named above; an argument that names none is the same for every part. Nothing has to cross between parts.
Inputs may be any that keep to these rules, and one draw needn't show every extreme that they name: tokens' feature scales differ by column and by sequence.
All inputs are finite; a program needn't handle non-finite values.
Results may differ from the reference program's by a relative error of at most 0.029.
Values may be sent and summed in bfloat16 or wider, within the bound.
A program may use at most 64 MiB of HBM per device.

```python
import jax
import jax.numpy as jnp
from jax import lax

D = 4096
NH = 32
DQK = 64
DV = 128
FF = 11264
SEQS = 64
N_TP = 4


def draw_tokens(key, part):
    base_key, col_key, row_key = jax.random.split(jax.random.fold_in(key, 11), 3)
    columns = jnp.arange(D, dtype=jnp.float32) / (D - 1)
    col_scale = 0.1 * 10.0 ** columns * jax.random.uniform(col_key, (D,), jnp.float32, 0.7, 1.3)
    row_factor = 10.0 ** (jax.random.uniform(row_key, (SEQS, 1), jnp.float32) - 0.5)
    base = jnp.clip(jax.random.normal(base_key, (SEQS, D), jnp.float32), -4.0, 4.0)
    return (base * col_scale[None, :] * row_factor).astype(jnp.bfloat16)


def draw_stabilizer(key, part):
    base_key = jax.random.fold_in(jax.random.fold_in(key, 23), 0)
    base = jax.random.uniform(base_key, (SEQS, NH), jnp.float32, -4.0, 4.0)
    return base


def raised(array, key, source, target, parts, factor):
    def block_of(position):
        return (jnp.arange(array.shape[position]) // (array.shape[position] // parts)).reshape((-1,) + (1,) * (array.ndim - 1 - position))

    near = jax.random.permutation(key, parts)[block_of(target)]
    second = (block_of(target) + parts // 2) % parts
    return jnp.where((block_of(source) == near) | (block_of(source) == second), factor * array, array)


def block_scale(own_key, extent, shards, least, top_value):
    def one(position, shards_of):
        steps = jax.random.uniform(jax.random.fold_in(jax.random.fold_in(own_key, 6), position), (shards_of,), jnp.float32, least / len(shards), top_value / len(shards))
        return jnp.repeat(jnp.exp(steps), extent[position] // shards_of).reshape((-1,) + (1,) * (len(extent) - position - 1))

    gain = one(*shards[0])
    for cut in shards[1:]:
        gain = gain * one(*cut)
    return gain


def gaussian(rng, shape, spread, most, cuts=(), kind=jnp.bfloat16):
    result = spread * jax.random.normal(rng, shape, jnp.float32)
    if cuts:
        result = result * block_scale(rng, shape, cuts, -0.22, 0.18)
    return jnp.clip(result, -most, most).astype(kind)


def noise_with(key, shape, deviation, most, cuts, heavy, kind=jnp.bfloat16):
    array = deviation * jax.random.normal(key, shape, jnp.float32)
    if cuts:
        array = array * block_scale(key, shape, cuts, -0.22, 0.18)
    return jnp.clip(raised(array, jax.random.fold_in(key, 3), *heavy), -most, most).astype(kind)


def setup_inputs(seed: int = 0, part: int = 0) -> dict:
    key_of = jax.random.split(jax.random.key(seed), 17)
    part_keys = jax.random.split(jax.random.fold_in(key_of[16], part), 17)
    return {
        "tokens": draw_tokens(jax.random.fold_in(jax.random.fold_in(key_of[16], part), 71), part),
        "norm_gain": jnp.clip(1.0 + 0.18 * jax.random.normal(key_of[1], (D,), jnp.float32), 0.099609375, 1.8984375).astype(jnp.bfloat16),
        "w_query": gaussian(key_of[2], (D, NH * DQK), D ** -0.5, 0.09375, ((0, 4), (1, 4))),
        "w_key": gaussian(key_of[3], (D, NH * DQK), D ** -0.5, 0.09375, ((0, 4), (1, 4))),
        "w_value": gaussian(key_of[4], (D, NH * DV), D ** -0.5, 0.09375, ((0, 4), (1, 4))),
        "w_outgate": gaussian(key_of[5], (D, NH * DV), D ** -0.5, 0.09375, ((0, 4), (1, 4))),
        "w_input_gate": gaussian(key_of[6], (D, NH), D ** -0.5, 0.09375, ((0, 4),)),
        "w_forget_gate": gaussian(key_of[7], (D, NH), D ** -0.5, 0.09375, ((0, 4),)),
        "memory": gaussian(part_keys[8], (SEQS, NH, DQK, DV), 0.5, 4.0, ((0, 4), (1, 4)), jnp.float32),
        "normalizer": gaussian(part_keys[9], (SEQS, NH, DQK), 0.5, 4.0, ((0, 4), (1, 4)), jnp.float32),
        "stabilizer": draw_stabilizer(jax.random.fold_in(jax.random.fold_in(key_of[16], part), 71), part),
        "w_mix_out": gaussian(key_of[11], (NH * DV, D), (NH * DV) ** -0.5, 0.09375, ((0, 4), (1, 4))),
        "ffn_gain": jnp.clip(1.0 + 0.18 * jax.random.normal(key_of[12], (D,), jnp.float32), 0.099609375, 1.8984375).astype(jnp.bfloat16),
        "w_gate": gaussian(key_of[13], (D, FF), D ** -0.5, 0.09375, ((0, 4), (1, 4))),
        "w_up": gaussian(key_of[14], (D, FF), D ** -0.5, 0.09375, ((0, 4), (1, 4))),
        "w_down": noise_with(key_of[15], (FF, D), (FF // 16) ** -0.5, 0.3125, ((0, 4), (1, 4)), (0, 1, 4, 2.0)),
    }


def row_scale(values):
    wide = values.astype(jnp.float32)
    return lax.rsqrt(lax.optimization_barrier(jnp.mean(wide * wide, axis=-1, keepdims=True)) + 1e-06)

def block_sum(left, right, blocks):
    rows = left.shape[0]
    inner = left.shape[1] // blocks
    left_b = left.reshape(rows, blocks, inner).transpose(1, 0, 2)
    right_b = right.reshape(blocks, inner, right.shape[1])

    def one_block(pair):
        partial_value = jnp.dot(pair[0], pair[1], preferred_element_type=jnp.float32)
        return partial_value.astype(jnp.bfloat16).astype(jnp.float32)
    return lax.optimization_barrier(jnp.sum(lax.map(one_block, (left_b, right_b)), axis=0))

def reference(tokens, norm_gain, w_query, w_key, w_value, w_outgate, w_input_gate, w_forget_gate, memory, normalizer, stabilizer, w_mix_out, ffn_gain, w_gate, w_up, w_down):
    seqs = tokens.shape[0]
    scale1 = row_scale(tokens)
    normed1 = (tokens.astype(jnp.float32) * norm_gain.astype(jnp.float32)).astype(jnp.bfloat16)

    def project(weight):
        return scale1 * jnp.dot(normed1, weight, preferred_element_type=jnp.float32)
    query = project(w_query).reshape(seqs, NH, DQK) * DQK ** (-0.5)
    key = project(w_key).reshape(seqs, NH, DQK)
    value = project(w_value).reshape(seqs, NH, DV)
    outgate = project(w_outgate)
    igate = project(w_input_gate)
    lforget = jax.nn.log_sigmoid(project(w_forget_gate))
    new_stabilizer = jnp.maximum(lforget + stabilizer, igate)
    decay = jnp.exp(lforget + stabilizer - new_stabilizer)
    inflow = jnp.exp(igate - new_stabilizer)
    new_memory = decay[:, :, None, None] * memory + inflow[:, :, None, None] * key[:, :, :, None] * value[:, :, None, :]
    new_normalizer = decay[:, :, None] * normalizer + inflow[:, :, None] * key
    numer = jnp.einsum('bhd,bhde->bhe', query, new_memory)
    denom = lax.optimization_barrier(jnp.sum(query * new_normalizer, axis=-1))
    readout = numer / jnp.maximum(jnp.abs(denom), jnp.exp(-new_stabilizer))[:, :, None]
    gated = (jax.nn.sigmoid(outgate) * readout.reshape(seqs, NH * DV)).astype(jnp.bfloat16)
    mixed_in = (tokens.astype(jnp.float32) + block_sum(gated, w_mix_out, N_TP)).astype(jnp.bfloat16)
    scale2 = row_scale(mixed_in)
    normed2 = (mixed_in.astype(jnp.float32) * ffn_gain.astype(jnp.float32)).astype(jnp.bfloat16)
    gate_pre = scale2 * jnp.dot(normed2, w_gate, preferred_element_type=jnp.float32)
    up_pre = scale2 * jnp.dot(normed2, w_up, preferred_element_type=jnp.float32)
    hidden = (jax.nn.silu(gate_pre) * up_pre).astype(jnp.bfloat16)
    layer_out = (mixed_in.astype(jnp.float32) + block_sum(hidden, w_down, N_TP)).astype(jnp.bfloat16)
    return (layer_out, new_memory, new_normalizer, new_stabilizer)
```

```python
import functools

import jax
import jax.numpy as jnp
from jax import lax
from jax.experimental import pallas as pl
from jax.experimental.pallas import tpu as pltpu
from jax.sharding import PartitionSpec as P

D = 4096
DQK = 64
DV = 128
F32 = jnp.float32
BF16 = jnp.bfloat16
MESH = pl.DeviceIdType.MESH
VMEM_LIMIT = 60 * 1024 * 1024


def remote(src, dst, send_sem, recv_sem, **device):
    return pltpu.make_async_remote_copy(
        src_ref=src, dst_ref=dst, send_sem=send_sem, recv_sem=recv_sem,
        device_id=device, device_id_type=MESH,
    )


class Place:
    def __init__(self, nkv, ntp):
        self.nkv, self.ntp, self.ny = nkv, ntp, nkv // 2
        self.kv = lax.axis_index("kv")
        self.tp = lax.axis_index("tp")
        self.y = self.kv // 2
        self.core = self.kv % 2
        self.pending = []

    def mate(self):
        return 2 * self.y + (1 - self.core)

    def barrier(self):
        sem = pltpu.get_barrier_semaphore()
        count = 0
        for d in range(1, self.ntp):
            pl.semaphore_signal(sem, inc=1, device_id={"tp": (self.tp + d) % self.ntp}, device_id_type=MESH)
            count += 1
        pl.semaphore_signal(sem, inc=1, device_id={"kv": self.mate()}, device_id_type=MESH)
        count += 1
        for d in range(1, self.ny):
            other = 2 * ((self.y + d) % self.ny) + self.core
            pl.semaphore_signal(sem, inc=1, device_id={"kv": other}, device_id_type=MESH)
            count += 1
        pl.semaphore_wait(sem, count)

    def send(self, copy):
        copy.start()
        self.pending.append(copy)

    def finish(self):
        for copy in self.pending:
            copy.wait_send()

    def tp_send_all(self, src_of, slots, ssem, rsem):
        for d in range(1, self.ntp):
            to = (self.tp + d) % self.ntp
            self.send(remote(src_of(to), slots.at[self.tp], ssem.at[to], rsem.at[self.tp], tp=to))

    def tp_wait_all(self, slots, ssem, rsem):
        for d in range(1, self.ntp):
            to = (self.tp + self.ntp - d) % self.ntp
            remote(slots.at[to], slots.at[to], ssem.at[to], rsem.at[to], tp=to).wait_recv()


class Scatter:
    def __init__(self, place, acc, r1, s2, r2, sems, g):
        self.p, self.acc, self.r1, self.s2, self.r2 = place, acc, r1, s2, r2
        self.d_s, self.d_r, self.y_s, self.y_r = (s.at[g] for s in sems)

    def start(self):
        p = self.p
        for d in range(1, p.ny + 1):
            y = (p.y + d) % p.ny
            p.send(remote(self.acc.at[2 * y + (1 - p.core)], self.r1.at[y], self.d_s.at[y], self.d_r.at[y], kv=p.mate()))

    def chip_sum(self, y):
        p = self.p
        remote(self.r1.at[y], self.r1.at[y], self.d_s.at[y], self.d_r.at[y], kv=p.mate()).wait_recv()
        return self.acc[2 * y + p.core] + self.r1[y]

    def middle(self):
        p = self.p
        for d in range(1, p.ny):
            y = (p.y + d) % p.ny
            self.s2[y] = self.chip_sum(y).astype(self.s2.dtype)
            p.send(remote(self.s2.at[y], self.r2.at[p.y], self.y_s.at[y], self.y_r.at[p.y], kv=2 * y + p.core))

    def end(self):
        p = self.p
        total = self.chip_sum(p.y)
        for d in range(1, p.ny):
            y = (p.y + p.ny - d) % p.ny
            remote(self.r2.at[y], self.r2.at[y], self.y_s.at[y], self.y_r.at[y], kv=2 * y + p.core).wait_recv()
            total = total + self.r2[y].astype(F32)
        return total


def scatter_scratch(nkv, own, n, dtype):
    ny = nkv // 2
    return [
        pltpu.VMEM((nkv, own, n), F32),
        pltpu.VMEM((ny, own, n), F32),
        pltpu.VMEM((ny, own, n), dtype),
        pltpu.VMEM((ny, own, n), dtype),
    ]


def scatter_sems(groups, ny):
    return [pltpu.SemaphoreType.DMA((groups, ny))] * 4


class Gather:
    def __init__(self, place, slots, sems, g):
        self.p, self.slots = place, slots
        self.y_s, self.y_r, self.d_s, self.d_r = (s.at[g] for s in sems)

    def start(self):
        p, mine = self.p, self.slots.at[self.p.kv]
        for d in range(1, p.ny):
            y = (p.y + d) % p.ny
            p.send(remote(mine, mine, self.y_s.at[y], self.y_r.at[p.y], kv=2 * y + p.core))
        p.send(remote(mine, mine, self.d_s.at[p.y], self.d_r.at[p.y], kv=p.mate()))

    def relay(self):
        p = self.p
        for d in range(1, p.ny):
            y = (p.y + p.ny - d) % p.ny
            slot = self.slots.at[2 * y + p.core]
            remote(slot, slot, self.y_s.at[y], self.y_r.at[y], kv=2 * y + p.core).wait_recv()
            p.send(remote(slot, slot, self.d_s.at[y], self.d_r.at[y], kv=p.mate()))

    def end(self):
        p = self.p
        for d in range(p.ny):
            y = (p.y + p.ny - d) % p.ny
            slot = self.slots.at[2 * y + 1 - p.core]
            remote(slot, slot, self.d_s.at[y], self.d_r.at[y], kv=p.mate()).wait_recv()


def normalize(place, pieces, gain, normed):
    cw = pieces.shape[2]
    squares = None
    for t in range(place.ntp):
        wide = pieces[t].astype(F32)
        normed[:, t * cw:(t + 1) * cw] = (wide * gain[:, t * cw:(t + 1) * cw].astype(F32)).astype(BF16)
        part = jnp.sum(wide * wide, axis=1, keepdims=True)
        squares = part if squares is None else squares + part
    return squares


def load(pairs, sems):
    copies = [pltpu.make_async_copy(src, dst, sems.at[i]) for i, (src, dst) in enumerate(pairs)]
    for copy in copies:
        copy.start()
    return copies


def project_kernel(nkv, ntp, tokens, gain, *refs):
    hbm, outs, refs = refs[:6], refs[6:11], refs[11:]
    vmem, (pieces, normed, load_sem, tp_s, tp_r), refs = refs[:6], refs[6:11], refs[11:]
    groups, sems = refs[:20], refs[20:24]
    own = tokens.shape[0] // nkv
    loads = load(list(zip(hbm, vmem)), load_sem)
    place = Place(nkv, ntp)
    place.barrier()
    place.tp_send_all(lambda to: tokens, pieces, tp_s, tp_r)
    pieces[place.tp] = tokens[...]
    place.tp_wait_all(pieces, tp_s, tp_r)
    squares = normalize(place, pieces, gain, normed)
    scatters = [Scatter(place, *groups[4 * g:4 * g + 4], sems, g) for g in range(5)]

    def split(value):
        return value.reshape(nkv, own, value.shape[1])

    small = groups[16]
    nh = vmem[4].shape[1]
    small[:, :, 2 * nh:] = split(jnp.broadcast_to(squares, (nkv * own, small.shape[2] - 2 * nh)))
    for g, at in ((4, 0), (5, nh)):
        loads[g].wait()
        small[:, :, at:at + nh] = split(jnp.dot(normed[...], vmem[g][...], preferred_element_type=F32))
    scatters[4].start()
    for g in range(4):
        loads[g].wait()
        groups[4 * g][...] = split(jnp.dot(normed[...], vmem[g][...], preferred_element_type=F32))
        scatters[g].start()
        scatters[g - 1 if g else 4].middle()
    scatters[3].middle()
    for g in (4, 0, 1, 2, 3):
        outs[g][...] = scatters[g].end()
    place.finish()


def mixer_kernel(nkv, ntp, chunks, gated, tokens, gain, *refs):
    hbm, out, refs = refs[:4], refs[4], refs[5:]
    (w_mix, w_gate, w_up, w_down), refs = refs[:4], refs[4:]
    (g_all, m_out, m_in, mine, pieces, normed, d_out, d_in, total, load_sem), refs = refs[:10], refs[10:]
    m_s, m_r, x_s, x_r, l_s, l_r = refs[:6]
    refs = refs[6:]
    n = len(chunks)
    small, refs = refs[:4], refs[4:]
    groups, refs = refs[:4 * n], refs[4 * n:]
    halls, refs = refs[:n], refs[n:]
    scatter_s, gather_s = refs[:4], refs[4:8]
    rows, cw = tokens.shape
    own = rows // nkv
    wide_n = nkv * own

    loads = load(list(zip(hbm, (w_mix, w_gate, w_up, w_down))), load_sem)
    place = Place(nkv, ntp)
    g_all[place.kv] = gated[...]
    place.barrier()
    first = Gather(place, g_all, gather_s, n)
    first.start()
    first.relay()
    first.end()
    loads[0].wait()

    def scatter_tp(value, outgoing, incoming, ssem, rsem):
        for t in range(ntp):
            outgoing[t] = value[:, t * cw:(t + 1) * cw].astype(BF16)
        place.tp_send_all(lambda to: outgoing.at[to], incoming, ssem, rsem)
        place.tp_wait_all(incoming, ssem, rsem)
        result = outgoing[place.tp].astype(F32)
        for d in range(1, ntp):
            result = result + incoming[(place.tp + d) % ntp].astype(F32)
        return result

    mix = jnp.dot(g_all[...].reshape(wide_n, g_all.shape[2]), w_mix[...], preferred_element_type=F32)
    mixed = (tokens[...].astype(F32) + scatter_tp(mix, m_out, m_in, m_s, m_r)).astype(BF16)
    mine[...] = mixed
    pieces[place.tp] = mixed
    place.tp_send_all(lambda to: mine, pieces, x_s, x_r)
    place.tp_wait_all(pieces, x_s, x_r)
    squares = normalize(place, pieces, gain, normed)
    small[0][...] = jnp.broadcast_to(squares, (wide_n, small[0].shape[2])).reshape(nkv, own, small[0].shape[2])
    sq = Scatter(place, *small, scatter_s, n)
    sq.start()
    loads[1].wait()
    loads[2].wait()
    scatters = [Scatter(place, *groups[4 * i:4 * i + 4], scatter_s, i) for i in range(n)]
    gathers = [Gather(place, halls[i], gather_s, i) for i in range(n)]
    for i, (at, w) in enumerate(chunks):
        acc = groups[4 * i]
        acc[:, :, :w] = jnp.dot(normed[...], w_gate[:, at:at + w], preferred_element_type=F32).reshape(nkv, own, w)
        acc[:, :, w:] = jnp.dot(normed[...], w_up[:, at:at + w], preferred_element_type=F32).reshape(nkv, own, w)
        scatters[i].start()
        if i == 0:
            sq.middle()
        else:
            scatters[i - 1].middle()
    scatters[n - 1].middle()
    scale2 = lax.rsqrt(sq.end()[:, :1] / D + 1e-06)
    for i, (at, w) in enumerate(chunks):
        both = scatters[i].end() * scale2
        halls[i][place.kv] = (jax.nn.silu(both[:, :w]) * both[:, w:]).astype(BF16)
        gathers[i].start()
        if i:
            gathers[i - 1].relay()
    loads[3].wait()
    for i, (at, w) in enumerate(chunks):
        if i == n - 1:
            gathers[i].relay()
        gathers[i].end()
        part = jnp.dot(halls[i][...].reshape(wide_n, w), w_down[at:at + w, :], preferred_element_type=F32)
        total[...] = part if i == 0 else total[...] + part
    down = scatter_tp(total[...], d_out, d_in, l_s, l_r)
    out[...] = (mine[...].astype(F32) + down).astype(BF16)
    place.finish()


def column_chunks(width):
    unit = 256 if width % 256 == 0 else 128
    count = width // unit
    parts = min(4, count)
    chunks, at = [], 0
    for i in range(parts):
        w = unit * (count // parts + (1 if i < count % parts else 0))
        chunks.append((at, w))
        at += w
    return chunks


def shards(nkv, ntp, tokens, norm_gain, w_query, w_key, w_value, w_outgate, w_input_gate, w_forget_gate,
           memory, normalizer, stabilizer, w_mix_out, ffn_gain, w_gate, w_up, w_down):
    rows, cw = tokens.shape
    own = rows // nkv
    ny = nkv // 2
    depth = norm_gain.shape[0]
    local_heads = memory.shape[1]
    nh = w_input_gate.shape[1]
    weights = (w_query, w_key, w_value, w_outgate, w_input_gate, w_forget_gate)
    any_spec = pl.BlockSpec(memory_space=pl.ANY)
    vm = pl.BlockSpec(memory_space=pltpu.VMEM)
    dma = pltpu.SemaphoreType.DMA
    widths = [w.shape[1] for w in weights[:4]]
    small = 128
    scratch = [pltpu.VMEM(w.shape, BF16) for w in weights]
    scratch += [pltpu.VMEM((ntp, rows, cw), BF16), pltpu.VMEM((rows, depth), BF16), dma((6,)), dma((ntp,)), dma((ntp,))]
    for n in widths:
        scratch += scatter_scratch(nkv, own, n, BF16)
    scratch += scatter_scratch(nkv, own, small, F32)
    scratch += scatter_sems(5, ny)
    z_query, z_key, z_value, z_outgate, z_small = pl.pallas_call(
        functools.partial(project_kernel, nkv, ntp),
        out_shape=[jax.ShapeDtypeStruct((own, n), F32) for n in widths + [small]],
        in_specs=[vm, vm] + [any_spec] * 6,
        out_specs=[vm] * 5,
        scratch_shapes=scratch,
        compiler_params=pltpu.CompilerParams(collective_id=0, has_side_effects=True, vmem_limit_bytes=VMEM_LIMIT),
        name="project",
    )(tokens, norm_gain.reshape(1, depth), *weights)

    head_start = lax.axis_index("tp") * local_heads
    scale1 = lax.rsqrt(z_small[:, 2 * nh:2 * nh + 1] / D + 1e-06)
    query = (scale1 * z_query).reshape(own, local_heads, DQK) * DQK ** (-0.5)
    key = (scale1 * z_key).reshape(own, local_heads, DQK)
    value = (scale1 * z_value).reshape(own, local_heads, DV)
    outgate = scale1 * z_outgate
    igate = scale1 * lax.dynamic_slice_in_dim(z_small, head_start, local_heads, 1)
    lforget = jax.nn.log_sigmoid(scale1 * lax.dynamic_slice_in_dim(z_small, nh + head_start, local_heads, 1))
    new_stabilizer = jnp.maximum(lforget + stabilizer, igate)
    decay = jnp.exp(lforget + stabilizer - new_stabilizer)
    inflow = jnp.exp(igate - new_stabilizer)
    new_memory = (
        decay[:, :, None, None] * memory
        + inflow[:, :, None, None] * key[:, :, :, None] * value[:, :, None, :]
    )
    new_normalizer = decay[:, :, None] * normalizer + inflow[:, :, None] * key
    numer = jnp.sum(query[:, :, :, None] * new_memory, axis=2)
    denom = jnp.sum(query * new_normalizer, axis=-1)
    readout = numer / jnp.maximum(jnp.abs(denom), jnp.exp(-new_stabilizer))[:, :, None]
    gated = (jax.nn.sigmoid(outgate) * readout.reshape(own, local_heads * DV)).astype(BF16)

    chunks = column_chunks(w_gate.shape[1])
    n = len(chunks)
    mix_rows = gated.shape[1]
    piece = pltpu.VMEM((ntp, rows, cw), BF16)
    scratch = [pltpu.VMEM(w.shape, BF16) for w in (w_mix_out, w_gate, w_up, w_down)]
    scratch += [pltpu.VMEM((nkv, own, mix_rows), BF16), piece, piece, pltpu.VMEM((rows, cw), BF16), piece,
                pltpu.VMEM((rows, depth), BF16), piece, piece, pltpu.VMEM((rows, w_down.shape[1]), F32), dma((4,))]
    scratch += [dma((ntp,))] * 6
    scratch += scatter_scratch(nkv, own, small, F32)
    for _, w in chunks:
        scratch += scatter_scratch(nkv, own, 2 * w, BF16)
    scratch += [pltpu.VMEM((nkv, own, w), BF16) for _, w in chunks]
    scratch += scatter_sems(n + 1, ny) + scatter_sems(n + 1, ny)
    layer_out = pl.pallas_call(
        functools.partial(mixer_kernel, nkv, ntp, chunks),
        out_shape=jax.ShapeDtypeStruct((rows, cw), BF16),
        in_specs=[vm, vm, vm] + [any_spec] * 4,
        out_specs=vm,
        scratch_shapes=scratch,
        compiler_params=pltpu.CompilerParams(collective_id=1, has_side_effects=True, vmem_limit_bytes=VMEM_LIMIT),
        name="mixer",
    )(gated, tokens, ffn_gain.reshape(1, depth), w_mix_out, w_gate, w_up, w_down)
    return (layer_out, new_memory, new_normalizer, new_stabilizer)


def solution(mesh):
    in_specs = (
        P("grp", ("kv", "tp")),
        P("kv"),
        P("kv", "tp"),
        P("kv", "tp"),
        P("kv", "tp"),
        P("kv", "tp"),
        P("kv", None),
        P("kv", None),
        P(("grp", "kv"), "tp", None, None),
        P(("grp", "kv"), "tp", None),
        P(("grp", "kv"), "tp"),
        P("tp", "kv"),
        P("kv"),
        P("kv", "tp"),
        P("kv", "tp"),
        P("tp", "kv"),
    )
    out_specs = (
        P("grp", ("kv", "tp")),
        P(("grp", "kv"), "tp", None, None),
        P(("grp", "kv"), "tp", None),
        P(("grp", "kv"), "tp"),
    )
    body = functools.partial(shards, mesh.shape["kv"], mesh.shape["tp"])
    return jax.shard_map(body, mesh=mesh, in_specs=in_specs, out_specs=out_specs, check_vma=False)
```

```python
import functools

import jax
import jax.numpy as jnp
from jax import lax
from jax.experimental import pallas as pl
from jax.experimental.pallas import tpu as pltpu
from jax.sharding import PartitionSpec as P

D = 4096
DQK = 64
DV = 128
F32 = jnp.float32
BF16 = jnp.bfloat16
MESH = pl.DeviceIdType.MESH
VMEM_LIMIT = 60 * 1024 * 1024


def remote(src, dst, send_sem, recv_sem, **device):
    return pltpu.make_async_remote_copy(
        src_ref=src, dst_ref=dst, send_sem=send_sem, recv_sem=recv_sem,
        device_id=device, device_id_type=MESH,
    )


class Place:
    def __init__(self, nkv, ntp):
        self.nkv, self.ntp, self.ny = nkv, ntp, nkv // 2
        self.kv = lax.axis_index("kv")
        self.tp = lax.axis_index("tp")
        self.y = self.kv // 2
        self.core = self.kv % 2
        self.pending = []

    def mate(self):
        return 2 * self.y + (1 - self.core)

    def barrier(self):
        sem = pltpu.get_barrier_semaphore()
        count = 0
        for d in range(1, self.ntp):
            pl.semaphore_signal(sem, inc=1, device_id={"tp": (self.tp + d) % self.ntp}, device_id_type=MESH)
            count += 1
        pl.semaphore_signal(sem, inc=1, device_id={"kv": self.mate()}, device_id_type=MESH)
        count += 1
        for d in range(1, self.ny):
            other = 2 * ((self.y + d) % self.ny) + self.core
            pl.semaphore_signal(sem, inc=1, device_id={"kv": other}, device_id_type=MESH)
            count += 1
        pl.semaphore_wait(sem, count)

    def send(self, copy):
        copy.start()
        self.pending.append(copy)

    def finish(self):
        for copy in self.pending:
            copy.wait_send()

    def tp_send_all(self, src_of, slots, ssem, rsem):
        for d in range(1, self.ntp):
            to = (self.tp + d) % self.ntp
            self.send(remote(src_of(to), slots.at[self.tp], ssem.at[to], rsem.at[self.tp], tp=to))

    def tp_wait_all(self, slots, ssem, rsem):
        for d in range(1, self.ntp):
            to = (self.tp + self.ntp - d) % self.ntp
            remote(slots.at[to], slots.at[to], ssem.at[to], rsem.at[to], tp=to).wait_recv()


class Scatter:
    def __init__(self, place, acc, r1, s2, r2, sems, g):
        self.p, self.acc, self.r1, self.s2, self.r2 = place, acc, r1, s2, r2
        self.d_s, self.d_r, self.y_s, self.y_r = (s.at[g] for s in sems)

    def start(self):
        p = self.p
        for d in range(1, p.ny + 1):
            y = (p.y + d) % p.ny
            p.send(remote(self.acc.at[2 * y + (1 - p.core)], self.r1.at[y], self.d_s.at[y], self.d_r.at[y], kv=p.mate()))

    def chip_sum(self, y):
        p = self.p
        remote(self.r1.at[y], self.r1.at[y], self.d_s.at[y], self.d_r.at[y], kv=p.mate()).wait_recv()
        return self.acc[2 * y + p.core] + self.r1[y]

    def middle(self):
        p = self.p
        for d in range(1, p.ny):
            y = (p.y + d) % p.ny
            self.s2[y] = self.chip_sum(y).astype(self.s2.dtype)
            p.send(remote(self.s2.at[y], self.r2.at[p.y], self.y_s.at[y], self.y_r.at[p.y], kv=2 * y + p.core))

    def end(self):
        p = self.p
        total = self.chip_sum(p.y)
        for d in range(1, p.ny):
            y = (p.y + p.ny - d) % p.ny
            remote(self.r2.at[y], self.r2.at[y], self.y_s.at[y], self.y_r.at[y], kv=2 * y + p.core).wait_recv()
            total = total + self.r2[y].astype(F32)
        return total


def scatter_scratch(nkv, own, n, dtype):
    ny = nkv // 2
    return [
        pltpu.VMEM((nkv, own, n), F32),
        pltpu.VMEM((ny, own, n), F32),
        pltpu.VMEM((ny, own, n), dtype),
        pltpu.VMEM((ny, own, n), dtype),
    ]


def scatter_sems(groups, ny):
    return [pltpu.SemaphoreType.DMA((groups, ny))] * 4


class Gather:
    def __init__(self, place, slots, sems, g):
        self.p, self.slots = place, slots
        self.y_s, self.y_r, self.d_s, self.d_r = (s.at[g] for s in sems)

    def start(self):
        p, mine = self.p, self.slots.at[self.p.kv]
        for d in range(1, p.ny):
            y = (p.y + d) % p.ny
            p.send(remote(mine, mine, self.y_s.at[y], self.y_r.at[p.y], kv=2 * y + p.core))
        p.send(remote(mine, mine, self.d_s.at[p.y], self.d_r.at[p.y], kv=p.mate()))

    def relay(self):
        p = self.p
        for d in range(1, p.ny):
            y = (p.y + p.ny - d) % p.ny
            slot = self.slots.at[2 * y + p.core]
            remote(slot, slot, self.y_s.at[y], self.y_r.at[y], kv=2 * y + p.core).wait_recv()
            p.send(remote(slot, slot, self.d_s.at[y], self.d_r.at[y], kv=p.mate()))

    def end(self):
        p = self.p
        for d in range(p.ny):
            y = (p.y + p.ny - d) % p.ny
            slot = self.slots.at[2 * y + 1 - p.core]
            remote(slot, slot, self.d_s.at[y], self.d_r.at[y], kv=p.mate()).wait_recv()


def normalize(place, pieces, gain, normed):
    cw = pieces.shape[2]
    gain = gain[...].astype(F32).reshape(1, gain.shape[0])
    squares = None
    for t in range(place.ntp):
        wide = pieces[t].astype(F32)
        normed[:, t * cw:(t + 1) * cw] = (wide * gain[:, t * cw:(t + 1) * cw]).astype(BF16)
        part = jnp.sum(wide * wide, axis=1, keepdims=True)
        squares = part if squares is None else squares + part
    return squares


def load(pairs, sems):
    copies = [pltpu.make_async_copy(src, dst, sems.at[i]) for i, (src, dst) in enumerate(pairs)]
    for copy in copies:
        copy.start()
    return copies


def project_kernel(nkv, ntp, tokens, gain, *refs):
    hbm, outs, refs = refs[:6], refs[6:11], refs[11:]
    vmem, (pieces, normed, load_sem, tp_s, tp_r), refs = refs[:6], refs[6:11], refs[11:]
    groups, sems = refs[:20], refs[20:24]
    own = tokens.shape[0] // nkv
    loads = load(list(zip(hbm, vmem)), load_sem)
    place = Place(nkv, ntp)
    place.barrier()
    place.tp_send_all(lambda to: tokens, pieces, tp_s, tp_r)
    pieces[place.tp] = tokens[...]
    place.tp_wait_all(pieces, tp_s, tp_r)
    squares = normalize(place, pieces, gain, normed)
    scatters = [Scatter(place, *groups[4 * g:4 * g + 4], sems, g) for g in range(5)]

    def split(value):
        return value.reshape(nkv, own, value.shape[1])

    small = groups[16]
    nh = vmem[4].shape[0]
    small[:, :, 2 * nh:] = split(jnp.broadcast_to(squares, (nkv * own, small.shape[2] - 2 * nh)))
    for g, at in ((4, 0), (5, nh)):
        loads[g].wait()
        small[:, :, at:at + nh] = split(lax.dot_general(
            normed[...], vmem[g][...], (((1,), (1,)), ((), ())), preferred_element_type=F32))
    scatters[4].start()
    for g in range(4):
        loads[g].wait()
        groups[4 * g][...] = split(jnp.dot(normed[...], vmem[g][...], preferred_element_type=F32))
        scatters[g].start()
        scatters[g - 1 if g else 4].middle()
    scatters[3].middle()
    for g in (4, 0, 1, 2, 3):
        outs[g][...] = scatters[g].end()
    place.finish()


def state_kernel(nh, ntp, zq, zk, zv, zo, zs, normalizer, stabilizer, memory,
                 new_memory, new_normalizer, new_stabilizer, gated, old, new, in_sem, out_sem):
    heads, own = stabilizer.shape
    loads = [pltpu.make_async_copy(memory.at[:, h], old.at[h], in_sem.at[h]) for h in range(heads)]
    for copy in loads:
        copy.start()
    tp = lax.axis_index("tp")
    scale1 = lax.rsqrt(zs[:, 2 * nh:2 * nh + 1] / D + 1e-06)

    def own_heads(at):
        value = zs[:, at:at + heads]
        for t in range(1, ntp):
            value = jnp.where(tp == t, zs[:, at + t * heads:at + (t + 1) * heads], value)
        return scale1 * value

    igate, forget = own_heads(0), own_heads(nh)
    lforget = jnp.minimum(forget, 0.0) - jnp.log1p(jnp.exp(-jnp.abs(forget)))
    kept = lforget + stabilizer[...].T
    stab = jnp.maximum(kept, igate)
    new_stabilizer[...] = stab.T
    decay, inflow, floor = jnp.exp(kept - stab), jnp.exp(igate - stab), jnp.exp(-stab)
    stores = []
    for h in range(heads):
        query = scale1 * zq[:, h * DQK:(h + 1) * DQK] * DQK ** (-0.5)
        key = inflow[:, h:h + 1] * (scale1 * zk[:, h * DQK:(h + 1) * DQK])
        value = scale1 * zv[:, h * DV:(h + 1) * DV]
        norm = decay[:, h:h + 1] * normalizer[:, h, :] + key
        new_normalizer[:, h, :] = norm
        denom = jnp.maximum(jnp.abs(jnp.sum(query * norm, axis=1, keepdims=True)), floor[:, h:h + 1])
        loads[h].wait()
        wide = jnp.broadcast_to(decay[:, h:h + 1], (own, DV))
        state = wide[:, None, :] * old[h] + key[:, :, None] * value[:, None, :]
        new[h] = state
        stores.append(pltpu.make_async_copy(new.at[h], new_memory.at[:, h], out_sem.at[h]))
        stores[h].start()
        numer = jnp.sum(query[:, :, None] * state, axis=1)
        out = jax.nn.sigmoid(scale1 * zo[:, h * DV:(h + 1) * DV]) * (numer / denom)
        gated[:, h * DV:(h + 1) * DV] = out.astype(BF16)
    for copy in stores:
        copy.wait()


def mixer_kernel(nkv, ntp, chunks, gated, tokens, gain, *refs):
    hbm, out, refs = refs[:4], refs[4], refs[5:]
    (w_mix, w_gate, w_up, w_down), refs = refs[:4], refs[4:]
    (g_all, m_out, m_in, mine, pieces, normed, d_out, d_in, total, load_sem), refs = refs[:10], refs[10:]
    m_s, m_r, x_s, x_r, l_s, l_r = refs[:6]
    refs = refs[6:]
    n = len(chunks)
    small, refs = refs[:4], refs[4:]
    groups, refs = refs[:4 * n], refs[4 * n:]
    halls, refs = refs[:n], refs[n:]
    scatter_s, gather_s = refs[:4], refs[4:8]
    rows, cw = tokens.shape
    own = rows // nkv
    wide_n = nkv * own

    loads = load(list(zip(hbm, (w_mix, w_gate, w_up, w_down))), load_sem)
    place = Place(nkv, ntp)
    g_all[place.kv] = gated[...]
    place.barrier()
    first = Gather(place, g_all, gather_s, n)
    first.start()
    first.relay()
    first.end()
    loads[0].wait()

    def scatter_tp(value, outgoing, incoming, ssem, rsem):
        for t in range(ntp):
            outgoing[t] = value[:, t * cw:(t + 1) * cw].astype(BF16)
        place.tp_send_all(lambda to: outgoing.at[to], incoming, ssem, rsem)
        place.tp_wait_all(incoming, ssem, rsem)
        result = outgoing[place.tp].astype(F32)
        for d in range(1, ntp):
            result = result + incoming[(place.tp + d) % ntp].astype(F32)
        return result

    mix = jnp.dot(g_all[...].reshape(wide_n, g_all.shape[2]), w_mix[...], preferred_element_type=F32)
    mixed = (tokens[...].astype(F32) + scatter_tp(mix, m_out, m_in, m_s, m_r)).astype(BF16)
    mine[...] = mixed
    pieces[place.tp] = mixed
    place.tp_send_all(lambda to: mine, pieces, x_s, x_r)
    place.tp_wait_all(pieces, x_s, x_r)
    squares = normalize(place, pieces, gain, normed)
    small[0][...] = jnp.broadcast_to(squares, (wide_n, small[0].shape[2])).reshape(nkv, own, small[0].shape[2])
    sq = Scatter(place, *small, scatter_s, n)
    sq.start()
    loads[1].wait()
    loads[2].wait()
    scatters = [Scatter(place, *groups[4 * i:4 * i + 4], scatter_s, i) for i in range(n)]
    gathers = [Gather(place, halls[i], gather_s, i) for i in range(n)]
    for i, (at, w) in enumerate(chunks):
        acc = groups[4 * i]
        acc[:, :, :w] = jnp.dot(normed[...], w_gate[:, at:at + w], preferred_element_type=F32).reshape(nkv, own, w)
        acc[:, :, w:] = jnp.dot(normed[...], w_up[:, at:at + w], preferred_element_type=F32).reshape(nkv, own, w)
        scatters[i].start()
        if i == 0:
            sq.middle()
        else:
            scatters[i - 1].middle()
    scatters[n - 1].middle()
    scale2 = lax.rsqrt(sq.end()[:, :1] / D + 1e-06)
    for i, (at, w) in enumerate(chunks):
        both = scatters[i].end() * scale2
        halls[i][place.kv] = (jax.nn.silu(both[:, :w]) * both[:, w:]).astype(BF16)
        gathers[i].start()
        if i:
            gathers[i - 1].relay()
    loads[3].wait()
    for i, (at, w) in enumerate(chunks):
        if i == n - 1:
            gathers[i].relay()
        gathers[i].end()
        part = jnp.dot(halls[i][...].reshape(wide_n, w), w_down[at:at + w, :], preferred_element_type=F32)
        total[...] = part if i == 0 else total[...] + part
    down = scatter_tp(total[...], d_out, d_in, l_s, l_r)
    out[...] = (mine[...].astype(F32) + down).astype(BF16)
    place.finish()


def column_chunks(width):
    unit = 256 if width % 256 == 0 else 128
    count = width // unit
    parts = min(4, count)
    chunks, at = [], 0
    for i in range(parts):
        w = unit * (count // parts + (1 if i < count % parts else 0))
        chunks.append((at, w))
        at += w
    return chunks


def shards(nkv, ntp, tokens, norm_gain, w_query, w_key, w_value, w_outgate, w_input_gate, w_forget_gate,
           memory, normalizer, stabilizer, w_mix_out, ffn_gain, w_gate, w_up, w_down):
    rows, cw = tokens.shape
    own = rows // nkv
    ny = nkv // 2
    depth = norm_gain.shape[0]
    local_heads = memory.shape[1]
    nh = w_input_gate.shape[1]
    weights = (w_query, w_key, w_value, w_outgate, w_input_gate.T, w_forget_gate.T)
    any_spec = pl.BlockSpec(memory_space=pl.ANY)
    vm = pl.BlockSpec(memory_space=pltpu.VMEM)
    dma = pltpu.SemaphoreType.DMA
    widths = [w.shape[1] for w in weights[:4]]
    small = 128
    scratch = [pltpu.VMEM(w.shape, BF16) for w in weights]
    scratch += [pltpu.VMEM((ntp, rows, cw), BF16), pltpu.VMEM((rows, depth), BF16), dma((6,)), dma((ntp,)), dma((ntp,))]
    for n in widths:
        scratch += scatter_scratch(nkv, own, n, BF16)
    scratch += scatter_scratch(nkv, own, small, F32)
    scratch += scatter_sems(5, ny)
    z_query, z_key, z_value, z_outgate, z_small = pl.pallas_call(
        functools.partial(project_kernel, nkv, ntp),
        out_shape=[jax.ShapeDtypeStruct((own, n), F32) for n in widths + [small]],
        in_specs=[vm, vm] + [any_spec] * 6,
        out_specs=[vm] * 5,
        scratch_shapes=scratch,
        compiler_params=pltpu.CompilerParams(collective_id=0, has_side_effects=True, vmem_limit_bytes=VMEM_LIMIT),
        name="project",
    )(tokens, norm_gain, *weights)

    hbm = pl.BlockSpec(memory_space=pltpu.HBM)
    new_memory, new_normalizer, new_stabilizer, gated = pl.pallas_call(
        functools.partial(state_kernel, nh, ntp),
        out_shape=[
            jax.ShapeDtypeStruct(memory.shape, F32),
            jax.ShapeDtypeStruct(normalizer.shape, F32),
            jax.ShapeDtypeStruct((local_heads, own), F32),
            jax.ShapeDtypeStruct((own, local_heads * DV), BF16),
        ],
        in_specs=[vm] * 7 + [hbm],
        out_specs=[hbm, vm, vm, vm],
        scratch_shapes=[
            pltpu.VMEM((local_heads, own, DQK, DV), F32),
            pltpu.VMEM((local_heads, own, DQK, DV), F32),
            dma((local_heads,)),
            dma((local_heads,)),
        ],
        compiler_params=pltpu.CompilerParams(vmem_limit_bytes=VMEM_LIMIT),
        name="state",
    )(z_query, z_key, z_value, z_outgate, z_small, normalizer, stabilizer.T, memory)
    new_stabilizer = new_stabilizer.T

    chunks = column_chunks(w_gate.shape[1])
    n = len(chunks)
    mix_rows = gated.shape[1]
    piece = pltpu.VMEM((ntp, rows, cw), BF16)
    scratch = [pltpu.VMEM(w.shape, BF16) for w in (w_mix_out, w_gate, w_up, w_down)]
    scratch += [pltpu.VMEM((nkv, own, mix_rows), BF16), piece, piece, pltpu.VMEM((rows, cw), BF16), piece,
                pltpu.VMEM((rows, depth), BF16), piece, piece, pltpu.VMEM((rows, w_down.shape[1]), F32), dma((4,))]
    scratch += [dma((ntp,))] * 6
    scratch += scatter_scratch(nkv, own, small, F32)
    for _, w in chunks:
        scratch += scatter_scratch(nkv, own, 2 * w, BF16)
    scratch += [pltpu.VMEM((nkv, own, w), BF16) for _, w in chunks]
    scratch += scatter_sems(n + 1, ny) + scatter_sems(n + 1, ny)
    layer_out = pl.pallas_call(
        functools.partial(mixer_kernel, nkv, ntp, chunks),
        out_shape=jax.ShapeDtypeStruct((rows, cw), BF16),
        in_specs=[vm, vm, vm] + [any_spec] * 4,
        out_specs=vm,
        scratch_shapes=scratch,
        compiler_params=pltpu.CompilerParams(collective_id=1, has_side_effects=True, vmem_limit_bytes=VMEM_LIMIT),
        name="mixer",
    )(gated, tokens, ffn_gain, w_mix_out, w_gate, w_up, w_down)
    return (layer_out, new_memory, new_normalizer, new_stabilizer)


def solution(mesh):
    in_specs = (
        P("grp", ("kv", "tp")),
        P("kv"),
        P("kv", "tp"),
        P("kv", "tp"),
        P("kv", "tp"),
        P("kv", "tp"),
        P("kv", None),
        P("kv", None),
        P(("grp", "kv"), "tp", None, None),
        P(("grp", "kv"), "tp", None),
        P(("grp", "kv"), "tp"),
        P("tp", "kv"),
        P("kv"),
        P("kv", "tp"),
        P("kv", "tp"),
        P("tp", "kv"),
    )
    out_specs = (
        P("grp", ("kv", "tp")),
        P(("grp", "kv"), "tp", None, None),
        P(("grp", "kv"), "tp", None),
        P(("grp", "kv"), "tp"),
    )
    body = functools.partial(shards, mesh.shape["kv"], mesh.shape["tp"])
    return jax.shard_map(body, mesh=mesh, in_specs=in_specs, out_specs=out_specs, check_vma=False)
```

```python
import functools

import jax
import jax.numpy as jnp
from jax import lax
from jax.experimental import pallas as pl
from jax.experimental.pallas import tpu as pltpu
from jax.sharding import PartitionSpec as P

D = 4096
DQK = 64
DV = 128
F32 = jnp.float32
BF16 = jnp.bfloat16
MESH = pl.DeviceIdType.MESH
VMEM_LIMIT = 60 * 1024 * 1024


def remote(src, dst, send_sem, recv_sem, **device):
    return pltpu.make_async_remote_copy(
        src_ref=src, dst_ref=dst, send_sem=send_sem, recv_sem=recv_sem,
        device_id=device, device_id_type=MESH,
    )


class Place:
    def __init__(self, nkv, ntp):
        self.nkv, self.ntp, self.ny = nkv, ntp, nkv // 2
        self.kv = lax.axis_index("kv")
        self.tp = lax.axis_index("tp")
        self.y = self.kv // 2
        self.core = self.kv % 2
        self.pending = []

    def mate(self):
        return 2 * self.y + (1 - self.core)

    def barrier(self):
        sem = pltpu.get_barrier_semaphore()
        count = 0
        for d in range(1, self.ntp):
            pl.semaphore_signal(sem, inc=1, device_id={"tp": (self.tp + d) % self.ntp}, device_id_type=MESH)
            count += 1
        pl.semaphore_signal(sem, inc=1, device_id={"kv": self.mate()}, device_id_type=MESH)
        count += 1
        for d in range(1, self.ny):
            other = 2 * ((self.y + d) % self.ny) + self.core
            pl.semaphore_signal(sem, inc=1, device_id={"kv": other}, device_id_type=MESH)
            count += 1
        pl.semaphore_wait(sem, count)

    def send(self, copy):
        copy.start()
        self.pending.append(copy)

    def finish(self):
        for copy in self.pending:
            copy.wait_send()

    def tp_send_all(self, src_of, slots, ssem, rsem):
        for d in range(1, self.ntp):
            to = (self.tp + d) % self.ntp
            self.send(remote(src_of(to), slots.at[self.tp], ssem.at[to], rsem.at[self.tp], tp=to))

    def tp_wait_all(self, slots, ssem, rsem):
        for d in range(1, self.ntp):
            to = (self.tp + self.ntp - d) % self.ntp
            remote(slots.at[to], slots.at[to], ssem.at[to], rsem.at[to], tp=to).wait_recv()


class Scatter:
    def __init__(self, place, acc, r1, s2, r2, sems, g):
        self.p, self.acc, self.r1, self.s2, self.r2 = place, acc, r1, s2, r2
        self.d_s, self.d_r, self.y_s, self.y_r = (s.at[g] for s in sems)

    def start(self):
        p = self.p
        for d in range(1, p.ny + 1):
            y = (p.y + d) % p.ny
            p.send(remote(self.acc.at[2 * y + (1 - p.core)], self.r1.at[y], self.d_s.at[y], self.d_r.at[y], kv=p.mate()))

    def chip_sum(self, y):
        p = self.p
        remote(self.r1.at[y], self.r1.at[y], self.d_s.at[y], self.d_r.at[y], kv=p.mate()).wait_recv()
        return self.acc[2 * y + p.core] + self.r1[y]

    def middle(self):
        p = self.p
        for d in range(1, p.ny):
            y = (p.y + d) % p.ny
            self.s2[y] = self.chip_sum(y).astype(self.s2.dtype)
            p.send(remote(self.s2.at[y], self.r2.at[p.y], self.y_s.at[y], self.y_r.at[p.y], kv=2 * y + p.core))

    def end(self):
        p = self.p
        total = self.chip_sum(p.y)
        for d in range(1, p.ny):
            y = (p.y + p.ny - d) % p.ny
            remote(self.r2.at[y], self.r2.at[y], self.y_s.at[y], self.y_r.at[y], kv=2 * y + p.core).wait_recv()
            total = total + self.r2[y].astype(F32)
        return total


def scatter_scratch(nkv, own, n, dtype):
    ny = nkv // 2
    return [
        pltpu.VMEM((nkv, own, n), F32),
        pltpu.VMEM((ny, own, n), F32),
        pltpu.VMEM((ny, own, n), dtype),
        pltpu.VMEM((ny, own, n), dtype),
    ]


def scatter_sems(groups, ny):
    return [pltpu.SemaphoreType.DMA((groups, ny))] * 4


class Gather:
    def __init__(self, place, slots, sems, g):
        self.p, self.slots = place, slots
        self.y_s, self.y_r, self.d_s, self.d_r = (s.at[g] for s in sems)

    def start(self):
        p, mine = self.p, self.slots.at[self.p.kv]
        for d in range(1, p.ny):
            y = (p.y + d) % p.ny
            p.send(remote(mine, mine, self.y_s.at[y], self.y_r.at[p.y], kv=2 * y + p.core))
        p.send(remote(mine, mine, self.d_s.at[p.y], self.d_r.at[p.y], kv=p.mate()))

    def relay(self):
        p = self.p
        for d in range(1, p.ny):
            y = (p.y + p.ny - d) % p.ny
            slot = self.slots.at[2 * y + p.core]
            remote(slot, slot, self.y_s.at[y], self.y_r.at[y], kv=2 * y + p.core).wait_recv()
            p.send(remote(slot, slot, self.d_s.at[y], self.d_r.at[y], kv=p.mate()))

    def end(self):
        p = self.p
        for d in range(p.ny):
            y = (p.y + p.ny - d) % p.ny
            slot = self.slots.at[2 * y + 1 - p.core]
            remote(slot, slot, self.d_s.at[y], self.d_r.at[y], kv=p.mate()).wait_recv()


def normalize(place, pieces, gain, normed):
    cw = pieces.shape[2]
    gain = gain[...].astype(F32).reshape(1, gain.shape[0])
    squares = None
    for t in range(place.ntp):
        wide = pieces[t].astype(F32)
        normed[:, t * cw:(t + 1) * cw] = (wide * gain[:, t * cw:(t + 1) * cw]).astype(BF16)
        part = jnp.sum(wide * wide, axis=1, keepdims=True)
        squares = part if squares is None else squares + part
    return squares


def load(pairs, sems):
    copies = [pltpu.make_async_copy(src, dst, sems.at[i]) for i, (src, dst) in enumerate(pairs)]
    for copy in copies:
        copy.start()
    return copies


def project_kernel(nkv, ntp, tokens, gain, *refs):
    hbm, outs, refs = refs[:6], refs[6:11], refs[11:]
    vmem, (pieces, normed, load_sem, tp_s, tp_r), refs = refs[:6], refs[6:11], refs[11:]
    groups, sems = refs[:20], refs[20:24]
    own = tokens.shape[0] // nkv
    loads = load(list(zip(hbm, vmem)), load_sem)
    place = Place(nkv, ntp)
    place.barrier()
    place.tp_send_all(lambda to: tokens, pieces, tp_s, tp_r)
    pieces[place.tp] = tokens[...]
    place.tp_wait_all(pieces, tp_s, tp_r)
    squares = normalize(place, pieces, gain, normed)
    scatters = [Scatter(place, *groups[4 * g:4 * g + 4], sems, g) for g in range(5)]

    def split(value):
        return value.reshape(nkv, own, value.shape[1])

    small = groups[16]
    nh = vmem[4].shape[0]
    small[:, :, 2 * nh:] = split(jnp.broadcast_to(squares, (nkv * own, small.shape[2] - 2 * nh)))
    for g, at in ((4, 0), (5, nh)):
        loads[g].wait()
        small[:, :, at:at + nh] = split(lax.dot_general(
            normed[...], vmem[g][...], (((1,), (1,)), ((), ())), preferred_element_type=F32))
    scatters[4].start()
    for g in range(4):
        loads[g].wait()
        groups[4 * g][...] = split(jnp.dot(normed[...], vmem[g][...], preferred_element_type=F32))
        scatters[g].start()
    for g in (4, 0, 1, 2, 3):
        scatters[g].middle()
    for g in (4, 0, 1, 2, 3):
        outs[g][...] = scatters[g].end()
    place.finish()


def state_kernel(nh, ntp, zq, zk, zv, zo, zs, normalizer, stabilizer, memory,
                 new_memory, new_normalizer, new_stabilizer, gated, old, new, in_sem, out_sem):
    heads, own = stabilizer.shape
    loads = [pltpu.make_async_copy(memory.at[:, h], old.at[h], in_sem.at[h]) for h in range(heads)]
    for copy in loads:
        copy.start()
    tp = lax.axis_index("tp")
    scale1 = lax.rsqrt(zs[:, 2 * nh:2 * nh + 1] / D + 1e-06)

    def own_heads(at):
        value = zs[:, at:at + heads]
        for t in range(1, ntp):
            value = jnp.where(tp == t, zs[:, at + t * heads:at + (t + 1) * heads], value)
        return scale1 * value

    igate, forget = own_heads(0), own_heads(nh)
    lforget = jnp.minimum(forget, 0.0) - jnp.log1p(jnp.exp(-jnp.abs(forget)))
    kept = lforget + stabilizer[...].T
    stab = jnp.maximum(kept, igate)
    new_stabilizer[...] = stab.T
    decay, inflow, floor = jnp.exp(kept - stab), jnp.exp(igate - stab), jnp.exp(-stab)
    stores = []
    for h in range(heads):
        query = scale1 * zq[:, h * DQK:(h + 1) * DQK] * DQK ** (-0.5)
        key = inflow[:, h:h + 1] * (scale1 * zk[:, h * DQK:(h + 1) * DQK])
        value = scale1 * zv[:, h * DV:(h + 1) * DV]
        norm = decay[:, h:h + 1] * normalizer[:, h, :] + key
        new_normalizer[:, h, :] = norm
        denom = jnp.maximum(jnp.abs(jnp.sum(query * norm, axis=1, keepdims=True)), floor[:, h:h + 1])
        loads[h].wait()
        wide = jnp.broadcast_to(decay[:, h:h + 1], (own, DV))
        state = wide[:, None, :] * old[h] + key[:, :, None] * value[:, None, :]
        new[h] = state
        stores.append(pltpu.make_async_copy(new.at[h], new_memory.at[:, h], out_sem.at[h]))
        stores[h].start()
        numer = jnp.sum(query[:, :, None] * state, axis=1)
        out = jax.nn.sigmoid(scale1 * zo[:, h * DV:(h + 1) * DV]) * (numer / denom)
        gated[:, h * DV:(h + 1) * DV] = out.astype(BF16)
    for copy in stores:
        copy.wait()


def mixer_kernel(nkv, ntp, chunks, gated, tokens, gain, *refs):
    hbm, out, refs = refs[:4], refs[4], refs[5:]
    (w_mix, w_gate, w_up, w_down), refs = refs[:4], refs[4:]
    (g_all, m_out, m_in, mine, pieces, normed, d_out, d_in, total, load_sem), refs = refs[:10], refs[10:]
    m_s, m_r, x_s, x_r, l_s, l_r = refs[:6]
    refs = refs[6:]
    n = len(chunks)
    small, refs = refs[:4], refs[4:]
    groups, refs = refs[:4 * n], refs[4 * n:]
    halls, refs = refs[:n], refs[n:]
    scatter_s, gather_s = refs[:4], refs[4:8]
    rows, cw = tokens.shape
    own = rows // nkv
    wide_n = nkv * own

    loads = load(list(zip(hbm, (w_mix, w_gate, w_up, w_down))), load_sem)
    place = Place(nkv, ntp)
    g_all[place.kv] = gated[...]
    place.barrier()
    first = Gather(place, g_all, gather_s, n)
    first.start()
    first.relay()
    first.end()
    loads[0].wait()

    def scatter_tp(value, outgoing, incoming, ssem, rsem):
        for t in range(ntp):
            outgoing[t] = value[:, t * cw:(t + 1) * cw].astype(BF16)
        place.tp_send_all(lambda to: outgoing.at[to], incoming, ssem, rsem)
        place.tp_wait_all(incoming, ssem, rsem)
        result = outgoing[place.tp].astype(F32)
        for d in range(1, ntp):
            result = result + incoming[(place.tp + d) % ntp].astype(F32)
        return result

    mix = jnp.dot(g_all[...].reshape(wide_n, g_all.shape[2]), w_mix[...], preferred_element_type=F32)
    mixed = (tokens[...].astype(F32) + scatter_tp(mix, m_out, m_in, m_s, m_r)).astype(BF16)
    mine[...] = mixed
    pieces[place.tp] = mixed
    place.tp_send_all(lambda to: mine, pieces, x_s, x_r)
    place.tp_wait_all(pieces, x_s, x_r)
    squares = normalize(place, pieces, gain, normed)
    small[0][...] = jnp.broadcast_to(squares, (wide_n, small[0].shape[2])).reshape(nkv, own, small[0].shape[2])
    sq = Scatter(place, *small, scatter_s, n)
    sq.start()
    loads[1].wait()
    loads[2].wait()
    scatters = [Scatter(place, *groups[4 * i:4 * i + 4], scatter_s, i) for i in range(n)]
    gathers = [Gather(place, halls[i], gather_s, i) for i in range(n)]
    for i, (at, w) in enumerate(chunks):
        acc = groups[4 * i]
        acc[:, :, :w] = jnp.dot(normed[...], w_gate[:, at:at + w], preferred_element_type=F32).reshape(nkv, own, w)
        acc[:, :, w:] = jnp.dot(normed[...], w_up[:, at:at + w], preferred_element_type=F32).reshape(nkv, own, w)
        scatters[i].start()
        if i == 0:
            sq.middle()
        else:
            scatters[i - 1].middle()
    scatters[n - 1].middle()
    scale2 = lax.rsqrt(sq.end()[:, :1] / D + 1e-06)
    for i, (at, w) in enumerate(chunks):
        both = scatters[i].end() * scale2
        halls[i][place.kv] = (jax.nn.silu(both[:, :w]) * both[:, w:]).astype(BF16)
        gathers[i].start()
    loads[3].wait()
    for gather in gathers:
        gather.relay()
    for i, (at, w) in enumerate(chunks):
        gathers[i].end()
        part = jnp.dot(halls[i][...].reshape(wide_n, w), w_down[at:at + w, :], preferred_element_type=F32)
        total[...] = part if i == 0 else total[...] + part
    down = scatter_tp(total[...], d_out, d_in, l_s, l_r)
    out[...] = (mine[...].astype(F32) + down).astype(BF16)
    place.finish()


def column_chunks(width):
    unit = 256 if width % 256 == 0 else 128
    count = width // unit
    parts = min(4, count)
    chunks, at = [], 0
    for i in range(parts):
        w = unit * (count // parts + (1 if i < count % parts else 0))
        chunks.append((at, w))
        at += w
    return chunks


def shards(nkv, ntp, tokens, norm_gain, w_query, w_key, w_value, w_outgate, w_input_gate, w_forget_gate,
           memory, normalizer, stabilizer, w_mix_out, ffn_gain, w_gate, w_up, w_down):
    rows, cw = tokens.shape
    own = rows // nkv
    ny = nkv // 2
    depth = norm_gain.shape[0]
    local_heads = memory.shape[1]
    nh = w_input_gate.shape[1]
    weights = (w_query, w_key, w_value, w_outgate, w_input_gate.T, w_forget_gate.T)
    any_spec = pl.BlockSpec(memory_space=pl.ANY)
    vm = pl.BlockSpec(memory_space=pltpu.VMEM)
    dma = pltpu.SemaphoreType.DMA
    widths = [w.shape[1] for w in weights[:4]]
    small = 128
    scratch = [pltpu.VMEM(w.shape, BF16) for w in weights]
    scratch += [pltpu.VMEM((ntp, rows, cw), BF16), pltpu.VMEM((rows, depth), BF16), dma((6,)), dma((ntp,)), dma((ntp,))]
    for n in widths:
        scratch += scatter_scratch(nkv, own, n, BF16)
    scratch += scatter_scratch(nkv, own, small, F32)
    scratch += scatter_sems(5, ny)
    z_query, z_key, z_value, z_outgate, z_small = pl.pallas_call(
        functools.partial(project_kernel, nkv, ntp),
        out_shape=[jax.ShapeDtypeStruct((own, n), F32) for n in widths + [small]],
        in_specs=[vm, vm] + [any_spec] * 6,
        out_specs=[vm] * 5,
        scratch_shapes=scratch,
        compiler_params=pltpu.CompilerParams(collective_id=0, has_side_effects=True, vmem_limit_bytes=VMEM_LIMIT),
        name="project",
    )(tokens, norm_gain, *weights)

    hbm = pl.BlockSpec(memory_space=pltpu.HBM)
    new_memory, new_normalizer, new_stabilizer, gated = pl.pallas_call(
        functools.partial(state_kernel, nh, ntp),
        out_shape=[
            jax.ShapeDtypeStruct(memory.shape, F32),
            jax.ShapeDtypeStruct(normalizer.shape, F32),
            jax.ShapeDtypeStruct((local_heads, own), F32),
            jax.ShapeDtypeStruct((own, local_heads * DV), BF16),
        ],
        in_specs=[vm] * 7 + [hbm],
        out_specs=[hbm, vm, vm, vm],
        scratch_shapes=[
            pltpu.VMEM((local_heads, own, DQK, DV), F32),
            pltpu.VMEM((local_heads, own, DQK, DV), F32),
            dma((local_heads,)),
            dma((local_heads,)),
        ],
        compiler_params=pltpu.CompilerParams(vmem_limit_bytes=VMEM_LIMIT),
        name="state",
    )(z_query, z_key, z_value, z_outgate, z_small, normalizer, stabilizer.T, memory)
    new_stabilizer = new_stabilizer.T

    chunks = column_chunks(w_gate.shape[1])
    n = len(chunks)
    mix_rows = gated.shape[1]
    piece = pltpu.VMEM((ntp, rows, cw), BF16)
    scratch = [pltpu.VMEM(w.shape, BF16) for w in (w_mix_out, w_gate, w_up, w_down)]
    scratch += [pltpu.VMEM((nkv, own, mix_rows), BF16), piece, piece, pltpu.VMEM((rows, cw), BF16), piece,
                pltpu.VMEM((rows, depth), BF16), piece, piece, pltpu.VMEM((rows, w_down.shape[1]), F32), dma((4,))]
    scratch += [dma((ntp,))] * 6
    scratch += scatter_scratch(nkv, own, small, F32)
    for _, w in chunks:
        scratch += scatter_scratch(nkv, own, 2 * w, BF16)
    scratch += [pltpu.VMEM((nkv, own, w), BF16) for _, w in chunks]
    scratch += scatter_sems(n + 1, ny) + scatter_sems(n + 1, ny)
    layer_out = pl.pallas_call(
        functools.partial(mixer_kernel, nkv, ntp, chunks),
        out_shape=jax.ShapeDtypeStruct((rows, cw), BF16),
        in_specs=[vm, vm, vm] + [any_spec] * 4,
        out_specs=vm,
        scratch_shapes=scratch,
        compiler_params=pltpu.CompilerParams(collective_id=1, has_side_effects=True, vmem_limit_bytes=VMEM_LIMIT),
        name="mixer",
    )(gated, tokens, ffn_gain, w_mix_out, w_gate, w_up, w_down)
    return (layer_out, new_memory, new_normalizer, new_stabilizer)


def solution(mesh):
    in_specs = (
        P("grp", ("kv", "tp")),
        P("kv"),
        P("kv", "tp"),
        P("kv", "tp"),
        P("kv", "tp"),
        P("kv", "tp"),
        P("kv", None),
        P("kv", None),
        P(("grp", "kv"), "tp", None, None),
        P(("grp", "kv"), "tp", None),
        P(("grp", "kv"), "tp"),
        P("tp", "kv"),
        P("kv"),
        P("kv", "tp"),
        P("kv", "tp"),
        P("tp", "kv"),
    )
    out_specs = (
        P("grp", ("kv", "tp")),
        P(("grp", "kv"), "tp", None, None),
        P(("grp", "kv"), "tp", None),
        P(("grp", "kv"), "tp"),
    )
    body = functools.partial(shards, mesh.shape["kv"], mesh.shape["tp"])
    return jax.shard_map(body, mesh=mesh, in_specs=in_specs, out_specs=out_specs, check_vma=False)
```
